32 devices in a mesh: sp: 8 (over z, y), tp: 4 (over x, core).
Axes of the slice: x: 2, y: 2, z: 4, core: 2. Of those that a mesh axis runs over, the one named last changes fastest.
Arguments:
- resid_stream: bfloat16 [3072, 2048], P('sp'), may hold values from -6 to 6
- q_latent: bfloat16 [3072, 512], P('sp'), may hold values from -6 to 6
- kv_latent: bfloat16 [3072, 256], P('sp'), may hold values from -6 to 6
- rope_key: bfloat16 [3072, 64], P('sp'), may hold values from -6 to 6
- doc_ids: int32 [3072], P('sp'), may hold values from 0 to 3, as said below
- q_gain: float32 [512], replicated, may hold values from 1.5 to 64
- kv_gain: float32 [256], replicated, may hold values from 0.1 to 1.9
- w_query: bfloat16 [512, 3072], P(None, 'tp'), may hold values from -0.25 to 0.25
- w_key: bfloat16 [256, 2048], P(None, 'tp'), may hold values from -0.375 to 0.375
- w_value: bfloat16 [256, 2048], P(None, 'tp'), may hold values from -0.375 to 0.375
- w_out: bfloat16 [2048, 2048], replicated, may hold values from -0.5 to 0.5
- mix_gain: float32 [2048], replicated, may hold values from 0.1 to 1.9
- w_gate: bfloat16 [2048, 5632], P('sp', 'tp'), may hold values from -0.125 to 0.125
- w_up: bfloat16 [2048, 5632], P('sp', 'tp'), may hold values from -0.125 to 0.125
- w_down: bfloat16 [5632, 2048], P('tp', 'sp'), may hold values from -0.3125 to 0.3125
- out_gain: float32 [2048], replicated, may hold values from 0.1 to 1.9
Outputs:
- layer_out: bfloat16 [3072, 2048], P(('sp', 'tp'))
The draws below stay inside these ranges and needn't reach their ends.
Inputs may be any that keep to these rules, and one draw needn't show every extreme that they name: `doc_ids`: document numbers never fall along the sequence; every document has 1 to 2304 positions and one has exactly 2304.
All inputs are finite; a program needn't handle non-finite values.
Results may differ from the reference program's by a relative error of at most 0.02.
The reference program's roundings to bfloat16 on the way count: a program that leaves them out, or rounds other values in their place, can miss the bound.
Values may be sent and summed in bfloat16 or wider, within the bound.
No kernel may reach another device: no remote copies, remote signals or barrier semaphores. Data moves between devices by JAX's collectives and lax.ppermute only.
A program may use at most 128 MiB of HBM per device.

```python
import math
import jax
import jax.numpy as jnp
from jax import lax

D = 2048
FF = 5632
HEADS = 16
NOPE = 128
RD = 64
VD = 128
QR = 512
KR = 256
TOK_DEV = 384
TOKENS = 3072
DOC_MOST = 2304
N_TP = 4


def draw_q_gain(key, part):
    return jnp.exp(jax.random.uniform(key, (QR,), jnp.float32, math.log(1.5), math.log(4.0)))


def draw_doc_ids(key, part):
    rest = TOKENS - DOC_MOST
    margin = max(1, rest // 6)
    key_slot = jax.random.fold_in(key, 11)
    key_first = jax.random.fold_in(key, 23)
    key_second = jax.random.fold_in(key, 37)
    big_slot = jax.random.randint(key_slot, (), 0, 4, dtype=jnp.int32)
    first_cut = jax.random.randint(key_first, (), margin, rest // 2, dtype=jnp.int32)
    second_cut = jax.random.randint(key_second, (), rest // 2 + margin, rest - margin + 1, dtype=jnp.int32)
    smaller = jnp.stack([first_cut, second_cut - first_cut, rest - second_cut]).astype(jnp.int32)
    slots = jnp.arange(4, dtype=jnp.int32)
    pick = slots - (slots > big_slot).astype(jnp.int32)
    pick = jnp.clip(pick, 0, 2)
    lengths = jnp.where(slots == big_slot, jnp.int32(DOC_MOST), jnp.take(smaller, pick))
    starts = jnp.cumsum(lengths).astype(jnp.int32)[:3]
    positions = jnp.arange(TOKENS, dtype=jnp.int32)
    return jnp.sum((positions[:, None] >= starts[None, :]).astype(jnp.int32), axis=1).astype(jnp.int32)


def shard_levels(stream_key, shape, split, low, largest):
    def one(axis_at, blocks):
        steps = jax.random.uniform(jax.random.fold_in(jax.random.fold_in(stream_key, 6), axis_at), (blocks,), jnp.float32, low / len(split), largest / len(split))
        return jnp.repeat(jnp.exp(steps), shape[axis_at] // blocks).reshape((-1,) + (1,) * (len(shape) - axis_at - 1))

    loudness = one(*split[0])
    for cut in split[1:]:
        loudness = loudness * one(*cut)
    return loudness


def normal_values(rng, dims, deviation, limit, shards=(), kind=jnp.bfloat16):
    values = jax.random.normal(rng, dims, jnp.float32) * deviation
    if len(shards) > 0:
        values = shard_levels(rng, dims, shards, -0.22, 0.18) * values
    return jnp.clip(values, min=-limit, max=limit).astype(kind)


def setup_inputs(seed: int = 0) -> dict:
    arg_keys = jax.random.split(jax.random.key(seed), 17)
    resid_stream = normal_values(arg_keys[0], (TOKENS, D), 1.0, 6.0, ((0, 8),))
    q_latent = normal_values(arg_keys[1], (TOKENS, QR), 1.0, 6.0, ((0, 8),))
    kv_latent = normal_values(arg_keys[2], (TOKENS, KR), 1.0, 6.0, ((0, 8),))
    rope_key = normal_values(arg_keys[3], (TOKENS, RD), 1.0, 6.0, ((0, 8),))
    doc_ids = draw_doc_ids(jax.random.fold_in(arg_keys[16], 71), 0)
    q_gain = draw_q_gain(jax.random.fold_in(arg_keys[16], 71), 0)
    kv_gain = jnp.clip(1.0 + 0.18 * jax.random.normal(arg_keys[6], (KR,), jnp.float32), 0.1, 1.9)
    w_query = normal_values(arg_keys[7], (QR, HEADS * (NOPE + RD)), QR ** -0.5, 0.25, ((1, 4),))
    w_key = normal_values(arg_keys[8], (KR, HEADS * NOPE), KR ** -0.5, 0.375, ((1, 4),))
    w_value = normal_values(arg_keys[9], (KR, HEADS * VD), KR ** -0.5, 0.375, ((1, 4),))
    w_out = normal_values(arg_keys[10], (HEADS * VD, D), (HEADS * VD // 16) ** -0.5, 0.5)
    mix_gain = jnp.clip(1.0 + 0.18 * jax.random.normal(arg_keys[11], (D,), jnp.float32), 0.1, 1.9)
    w_gate = normal_values(arg_keys[12], (D, FF), D ** -0.5, 0.125, ((0, 8), (1, 4)))
    w_up = normal_values(arg_keys[13], (D, FF), D ** -0.5, 0.125, ((0, 8), (1, 4)))
    w_down = normal_values(arg_keys[14], (FF, D), (FF // 16) ** -0.5, 0.3125, ((0, 4), (1, 8)))
    out_gain = jnp.clip(1.0 + 0.18 * jax.random.normal(arg_keys[15], (D,), jnp.float32), 0.1, 1.9)
    return dict(resid_stream=resid_stream, q_latent=q_latent, kv_latent=kv_latent, rope_key=rope_key, doc_ids=doc_ids, q_gain=q_gain, kv_gain=kv_gain, w_query=w_query, w_key=w_key, w_value=w_value, w_out=w_out, mix_gain=mix_gain, w_gate=w_gate, w_up=w_up, w_down=w_down, out_gain=out_gain)


eps_norm = 1e-05
rope_theta = 10000.0
resid_alpha = 8.0 ** 0.25

def rope_angles(positions):
    frequency = rope_theta ** (-jnp.arange(0, RD, 2, dtype=jnp.float32) / RD)
    angles = positions.astype(jnp.float32)[:, None] * frequency[None, :]
    return (jnp.cos(angles), jnp.sin(angles))

def rotate(values, cos_table, sin_table):
    half_width = values.shape[-1] // 2
    first_half = values[..., :half_width]
    second_half = values[..., half_width:]
    return jnp.concatenate([first_half * cos_table - second_half * sin_table, second_half * cos_table + first_half * sin_table], axis=-1)

def rms_scaled(latent, scaling):
    widened = latent.astype(jnp.float32)
    inverse = lax.rsqrt(lax.optimization_barrier(jnp.mean(widened * widened, axis=-1, keepdims=True)) + eps_norm)
    return (widened * inverse * scaling).astype(jnp.bfloat16)

def layer_scaled(stream, scaling):
    centre = stream - lax.optimization_barrier(jnp.mean(stream, axis=-1, keepdims=True))
    spread = lax.optimization_barrier(jnp.mean(centre * centre, axis=-1, keepdims=True))
    return centre * lax.rsqrt(spread + eps_norm) * scaling

def widen(packed):
    return lax.optimization_barrier(packed).astype(jnp.float32)

def reference(resid_stream, q_latent, kv_latent, rope_key, doc_ids, q_gain, kv_gain, w_query, w_key, w_value, w_out, mix_gain, w_gate, w_up, w_down, out_gain):
    positions = jnp.arange(TOKENS, dtype=jnp.int32)
    cos_table, sin_table = rope_angles(positions)
    q_normed = rms_scaled(q_latent, q_gain)
    queries = jnp.dot(q_normed, w_query, preferred_element_type=jnp.float32).reshape(TOKENS, HEADS, NOPE + RD)
    queries = jnp.concatenate([queries[:, :, :NOPE], rotate(queries[:, :, NOPE:], cos_table[:, None, :], sin_table[:, None, :])], axis=-1).astype(jnp.bfloat16)
    kv_normed = rms_scaled(kv_latent, kv_gain)
    key_nope = jnp.dot(kv_normed, w_key, preferred_element_type=jnp.float32).astype(jnp.bfloat16).reshape(TOKENS, HEADS, NOPE)
    values = jnp.dot(kv_normed, w_value, preferred_element_type=jnp.float32).astype(jnp.bfloat16).reshape(TOKENS, HEADS, VD)
    key_rot = rotate(rope_key.astype(jnp.float32), cos_table, sin_table).astype(jnp.bfloat16)
    score_scale = (NOPE + RD) ** (-0.5)
    key_wide = widen(key_nope)
    rot_wide = widen(key_rot)
    value_wide = widen(values)

    def one_block(block_index):
        first_row = (block_index * TOK_DEV).astype(jnp.int32)
        query_block = widen(lax.dynamic_slice_in_dim(queries, first_row, TOK_DEV, 0))
        doc_block = lax.dynamic_slice_in_dim(doc_ids, first_row, TOK_DEV, 0)
        scores = jnp.einsum('qhd,khd->hqk', query_block[:, :, :NOPE], key_wide)
        scores = (scores + jnp.einsum('qhd,kd->hqk', query_block[:, :, NOPE:], rot_wide)) * score_scale
        same_doc = (doc_block[:, None] == doc_ids[None, :])[None]
        masked = jnp.where(same_doc, scores, -1e+30)
        row_top = lax.optimization_barrier(jnp.max(masked, axis=-1, keepdims=True))
        weights = jnp.where(same_doc, jnp.exp(masked - row_top), 0.0)
        denom_sum = lax.optimization_barrier(jnp.sum(weights, axis=-1))
        weighted = jnp.einsum('hqk,khd->qhd', widen(weights.astype(jnp.bfloat16)), value_wide)
        return (weighted / jnp.transpose(denom_sum)[:, :, None]).astype(jnp.bfloat16)
    block_out = lax.map(one_block, jnp.arange(TOKENS // TOK_DEV, dtype=jnp.int32))
    attended = block_out.reshape(TOKENS, HEADS * VD)
    mixer_out = jnp.dot(attended, w_out, preferred_element_type=jnp.float32)
    normed_mid = layer_scaled(resid_alpha * resid_stream.astype(jnp.float32) + mixer_out, mix_gain).astype(jnp.bfloat16)
    gate_pre = jnp.dot(normed_mid, w_gate, preferred_element_type=jnp.float32)
    up_pre = jnp.dot(normed_mid, w_up, preferred_element_type=jnp.float32)
    hidden = (jax.nn.silu(gate_pre) * up_pre).astype(jnp.bfloat16)
    group_width = FF // N_TP
    ffn_sum = jnp.zeros((TOKENS, D), jnp.float32)
    for group_index in range(N_TP):
        partial_sum = jnp.dot(hidden[:, group_index * group_width:(group_index + 1) * group_width], w_down[group_index * group_width:(group_index + 1) * group_width, :], preferred_element_type=jnp.float32)
        ffn_sum = ffn_sum + widen(partial_sum.astype(jnp.bfloat16))
    layer_out = layer_scaled(resid_alpha * normed_mid.astype(jnp.float32) + 0.5 * ffn_sum, out_gain).astype(jnp.bfloat16)
    return layer_out
```

```python
import functools

import jax
import jax.numpy as jnp
from jax import lax
from jax.experimental import pallas as pl
from jax.experimental.pallas import tpu as pltpu
from jax.sharding import PartitionSpec as P

NOPE = 128
RD = 64
VD = 128
QW = 256
CORES = 2

eps_norm = 1e-05
rope_theta = 10000.0
resid_alpha = 8.0**0.25
LOG2E = 1.4426950408889634
NT = (((1,), (1,)), ((), ()))


def rope_angles(positions):
    frequency = rope_theta ** (-jnp.arange(0, RD, 2, dtype=jnp.float32) / RD)
    angles = positions.astype(jnp.float32)[:, None] * frequency[None, :]
    return (jnp.cos(angles), jnp.sin(angles))


def rotate(values, cos_table, sin_table):
    half_width = values.shape[-1] // 2
    first_half = values[..., :half_width]
    second_half = values[..., half_width:]
    return jnp.concatenate(
        [
            first_half * cos_table - second_half * sin_table,
            second_half * cos_table + first_half * sin_table,
        ],
        axis=-1,
    )


def rms_scaled(latent, scaling):
    widened = latent.astype(jnp.float32)
    inverse = lax.rsqrt(jnp.mean(widened * widened, axis=-1, keepdims=True) + eps_norm)
    return (widened * inverse * scaling).astype(jnp.bfloat16)


def layer_scaled(stream, scaling):
    centre = stream - jnp.mean(stream, axis=-1, keepdims=True)
    spread = jnp.mean(centre * centre, axis=-1, keepdims=True)
    return centre * lax.rsqrt(spread + eps_norm) * scaling


def attend_kernel(q_ref, lat_ref, rot_ref, qdoc_ref, kdoc_ref, wk_ref, wv_ref, out_ref, kcat, vals, *, tile):
    @pl.when(pl.program_id(0) == 0)
    def _():
        kcat[:, NOPE:] = rot_ref[...]

    lat = lat_ref[...]
    kcat[:, :NOPE] = jnp.dot(lat, wk_ref[...], preferred_element_type=jnp.float32).astype(jnp.bfloat16)
    vals[...] = jnp.dot(lat, wv_ref[...], preferred_element_type=jnp.float32).astype(jnp.bfloat16)
    factor = (NOPE + RD) ** (-0.5) * LOG2E
    for row in range(0, q_ref.shape[1], tile):
        rows = slice(row, row + tile)
        scores = lax.dot_general(q_ref[0, rows, :], kcat[...], NT, preferred_element_type=jnp.float32)
        scores = jnp.where(qdoc_ref[rows, :] == kdoc_ref[...], scores, -1e30)
        top = jnp.max(scores, axis=-1, keepdims=True)
        weights = jnp.exp2((scores - top) * factor)
        total = jnp.sum(weights, axis=-1, keepdims=True)
        mixed = jnp.dot(weights.astype(jnp.bfloat16), vals[...], preferred_element_type=jnp.float32)
        out_ref[rows, :] = (mixed / total).astype(jnp.bfloat16)


def attend(q, lat, rot, qdoc, kdoc, w_key, w_value):
    heads, rows, _ = q.shape
    keys, width = lat.shape
    tile = 128 if rows % 128 == 0 else rows
    return pl.pallas_call(
        functools.partial(attend_kernel, tile=tile),
        grid=(heads,),
        in_specs=[
            pl.BlockSpec((1, rows, QW), lambda i: (i, 0, 0)),
            pl.BlockSpec((keys, width), lambda i: (0, 0)),
            pl.BlockSpec((keys, QW - NOPE), lambda i: (0, 0)),
            pl.BlockSpec((rows, 1), lambda i: (0, 0)),
            pl.BlockSpec((1, keys), lambda i: (0, 0)),
            pl.BlockSpec((width, NOPE), lambda i: (0, i)),
            pl.BlockSpec((width, VD), lambda i: (0, i)),
        ],
        out_specs=pl.BlockSpec((rows, VD), lambda i: (0, i)),
        out_shape=jax.ShapeDtypeStruct((rows, heads * VD), jnp.bfloat16),
        scratch_shapes=[pltpu.VMEM((keys, QW), jnp.bfloat16), pltpu.VMEM((keys, VD), jnp.bfloat16)],
        compiler_params=pltpu.CompilerParams(vmem_limit_bytes=60 * 1024 * 1024),
        cost_estimate=pl.CostEstimate(
            flops=2 * heads * keys * (rows * (QW + VD) + width * (NOPE + VD)),
            bytes_accessed=2 * (heads * rows * QW + keys * (width + QW)),
            transcendentals=heads * rows * keys,
        ),
        name="attend",
    )(q, lat, rot, qdoc, kdoc, w_key, w_value)


def hidden_kernel(index_ref, xa_ref, xb_ref, *rest, n_pieces, tile):
    pieces = rest[:n_pieces]
    out_ref, gate_w, up_w, sems = rest[n_pieces:]
    units, width = pieces[0].shape
    units //= 2
    copies = []
    for i, piece in enumerate(pieces):
        place = pl.ds(pl.multiple_of(index_ref[i] * width, width), width)
        copies.append(pltpu.make_async_copy(piece.at[pl.ds(0, units)], gate_w.at[:, place], sems.at[2 * i]))
        copies.append(pltpu.make_async_copy(piece.at[pl.ds(units, units)], up_w.at[:, place], sems.at[2 * i + 1]))
    for copy in copies:
        copy.start()
    for copy in copies:
        copy.wait()
    half = xa_ref.shape[0]
    for base, x_ref in ((0, xa_ref), (half, xb_ref)):
        for row in range(0, half, tile):
            x = x_ref[row : row + tile, :]
            gate = lax.dot_general(x, gate_w[...], NT, preferred_element_type=jnp.float32)
            up = lax.dot_general(x, up_w[...], NT, preferred_element_type=jnp.float32)
            out_ref[base + row : base + row + tile, :] = (gate / (1.0 + jnp.exp(-gate)) * up).astype(jnp.bfloat16)


def hidden_units(index, xa, xb, pieces):
    units = pieces[0].shape[0] // 2
    half, width = xa.shape
    tile = 128 if half % 128 == 0 else half
    n = len(pieces)
    vmem = pl.BlockSpec(memory_space=pltpu.VMEM)
    return pl.pallas_call(
        functools.partial(hidden_kernel, n_pieces=n, tile=tile),
        in_specs=[pl.BlockSpec(memory_space=pltpu.SMEM), vmem, vmem] + [pl.BlockSpec(memory_space=pl.ANY)] * n,
        out_specs=vmem,
        out_shape=jax.ShapeDtypeStruct((2 * half, units), jnp.bfloat16),
        scratch_shapes=[
            pltpu.VMEM((units, width), jnp.bfloat16),
            pltpu.VMEM((units, width), jnp.bfloat16),
            pltpu.SemaphoreType.DMA((2 * n,)),
        ],
        compiler_params=pltpu.CompilerParams(vmem_limit_bytes=60 * 1024 * 1024),
        cost_estimate=pl.CostEstimate(
            flops=8 * half * units * width, bytes_accessed=4 * units * width + 4 * half * width, transcendentals=2 * half * units
        ),
        name="hidden_units",
    )(index, xa, xb, *pieces)


def body(
    resid_stream,
    q_latent,
    kv_latent,
    rope_key,
    doc_ids,
    q_gain,
    kv_gain,
    w_query,
    w_key,
    w_value,
    w_out,
    mix_gain,
    w_gate,
    w_up,
    w_down,
    out_gain,
):
    bf16 = jnp.bfloat16
    f32 = jnp.float32
    tok_rows = q_latent.shape[0]
    heads = w_key.shape[1] // NOPE
    n_sp = lax.axis_size("sp")
    n_tp = lax.axis_size("tp")
    n_x = n_tp // CORES
    n_y = n_x if n_sp % (2 * n_x) == 0 else 1
    n_h = 2
    n_l = n_sp // (n_h * n_y)
    sp = lax.axis_index("sp")
    tp = lax.axis_index("tp")
    at_y = sp % n_y
    at_l = (sp // n_y) % n_l
    at_h = sp // (n_y * n_l)
    at_core = tp % CORES
    d_block = w_gate.shape[0]
    ff_block = w_gate.shape[1]
    units = ff_block // n_l
    part_rows = tok_rows // n_tp
    half_rows = tok_rows // CORES

    def sp_move(value, dh, dl, dy):
        pairs = []
        for s in range(n_sp):
            y, l, h = s % n_y, (s // n_y) % n_l, s // (n_y * n_l)
            pairs.append((s, (((h + dh) % n_h) * n_l + (l + dl) % n_l) * n_y + (y + dy) % n_y))
        return lax.ppermute(value, "sp", pairs)

    def lx_move(value, dl, dx):
        pairs = []
        for s in range(n_sp):
            y, l, h = s % n_y, (s // n_y) % n_l, s // (n_y * n_l)
            to_sp = (h * n_l + (l + dl) % n_l) * n_y + y
            for t in range(n_tp):
                x, core = t // CORES, t % CORES
                pairs.append((s * n_tp + t, to_sp * n_tp + ((x + dx) % n_x) * CORES + core))
        return lax.ppermute(value, ("sp", "tp"), pairs)

    def core_swap(value):
        return lax.ppermute(value, "tp", [(t, t // CORES * CORES + (t + 1) % CORES) for t in range(n_tp)])

    z_steps = [(dh, dl) for dh in range(n_h) for dl in range(n_l)]

    positions = sp * tok_rows + jnp.arange(tok_rows, dtype=jnp.int32)
    cos_table, sin_table = rope_angles(positions)
    kv_normed = rms_scaled(kv_latent, kv_gain)
    key_rot = rotate(rope_key.astype(f32), cos_table, sin_table).astype(bf16)
    doc_code = jnp.stack([doc_ids // 128, doc_ids % 128], axis=1).astype(bf16)
    packed = jnp.concatenate([kv_normed, key_rot, doc_code], axis=1)
    packed = lax.dynamic_slice_in_dim(packed, at_core * half_rows, half_rows, 0)
    packs = [packed if (dh, dl) == (0, 0) else sp_move(packed, dh, dl, 0) for dh, dl in z_steps]
    packs = packs + [sp_move(p, 0, 0, dy) for p in packs for dy in range(1, n_y)]
    pack_half = jnp.concatenate(packs, axis=0)
    pack_all = jnp.concatenate([pack_half, core_swap(pack_half)], axis=0)
    key_width = kv_latent.shape[1]
    lat = pack_all[:, :key_width]
    rot = jnp.pad(pack_all[:, key_width : key_width + RD], ((0, 0), (0, QW - NOPE - RD)))
    codes = pack_all[:, key_width + RD :].astype(jnp.int32)
    kdoc = (codes[:, 0] * 128 + codes[:, 1])[None, :]

    def halves(weight):
        mine = lax.dynamic_slice_in_dim(weight, at_l * units, units, 0)
        return [mine] + [
            lax.dynamic_slice_in_dim(weight, ((at_l + dl) % n_l) * units, units, 0) for dl in range(1, n_l)
        ]

    gate_halves = halves(w_gate.T)
    up_halves = halves(w_up.T)
    gate_up = [jnp.concatenate([g, u], axis=0) for g, u in zip(gate_halves, up_halves)]
    down = halves(w_down)

    def spread(parts):
        over_z = [parts[dl] if (dh, dl) == (0, 0) else sp_move(parts[dl], dh, dl, 0) for dh, dl in z_steps]
        return {
            (dh, dl, dy): over_z[i] if dy == 0 else sp_move(over_z[i], 0, 0, dy)
            for i, (dh, dl) in enumerate(z_steps)
            for dy in range(n_y)
        }

    gate_up_pieces = spread(gate_up)
    down_pieces = spread(down)

    def block_of(dh, dl, dy):
        return (((at_h - dh) % n_h) * n_l + (at_l - dl) % n_l) * n_y + (at_y - dy) % n_y

    q_normed = rms_scaled(q_latent, q_gain)
    queries = jnp.dot(q_normed, w_query, preferred_element_type=f32).reshape(tok_rows, heads, NOPE + RD)
    turned = rotate(queries[:, :, NOPE:], cos_table[:, None, :], sin_table[:, None, :])
    q_rows = jnp.concatenate(
        [queries[:, :, :NOPE], turned, jnp.zeros((tok_rows, heads, QW - NOPE - RD), f32)], axis=-1
    ).astype(bf16)
    attended = attend(jnp.transpose(q_rows, (1, 0, 2)), lat, rot, doc_ids[:, None], kdoc, w_key, w_value)

    heads_rows = lax.all_to_all(attended, "tp", split_axis=0, concat_axis=1, tiled=True)
    mixer_out = jnp.dot(heads_rows, w_out, preferred_element_type=f32)
    own_resid = lax.dynamic_slice_in_dim(resid_stream, tp * part_rows, part_rows, 0)
    own_normed = layer_scaled(resid_alpha * own_resid.astype(f32) + mixer_out, mix_gain).astype(bf16)

    lx_steps = [(dl, dx) for dl in range(n_l) for dx in range(n_x)]
    rows_a = jnp.concatenate(
        [own_normed if step == (0, 0) else lx_move(own_normed, *step) for step in lx_steps], axis=0
    )
    rows_b = core_swap(rows_a)
    keys = [(dh, dl, dy) for dh, dl in z_steps for dy in range(n_y)]
    if d_block % 128 == 0:
        index = jnp.stack([block_of(*k) for k in keys]).astype(jnp.int32)
        hidden = hidden_units(index, rows_a, rows_b, [gate_up_pieces[k] for k in keys])
    else:
        gathered = jnp.zeros((n_sp, 2 * units, d_block), bf16)
        for k in keys:
            gathered = lax.dynamic_update_slice_in_dim(gathered, gate_up_pieces[k][None], block_of(*k), 0)
        weight = jnp.transpose(gathered, (1, 0, 2)).reshape(2 * units, n_sp * d_block)
        both = lax.dot_general(jnp.concatenate([rows_a, rows_b]), weight, NT, preferred_element_type=f32)
        hidden = (jax.nn.silu(both[:, :units]) * both[:, units:]).astype(bf16)

    group_rows = rows_a.shape[0]
    sums = {}
    chunks = [[(0, dy) for dy in range(n_y)]] + [[(dh, dy) for dh in range(1, n_h) for dy in range(n_y)]]
    for chunk in chunks:
        parts = []
        for dh, dy in chunk:
            outs = [jnp.dot(hidden, down_pieces[(dh, dl, dy)], preferred_element_type=f32) for dl in range(n_l)]
            stacked = jnp.stack(outs)
            parts.append(jnp.take(stacked, (at_l - jnp.arange(n_l)) % n_l, axis=0))
        partial = jnp.concatenate(parts, axis=0)
        other = core_swap(partial[:, group_rows:].astype(bf16))
        mine = (partial[:, :group_rows] + other.astype(f32)).astype(bf16)
        total = 0.0
        for i, (dl, dx) in enumerate(lx_steps):
            block = mine[:, i * part_rows : (i + 1) * part_rows]
            moved = block if (dl, dx) == (0, 0) else lx_move(block, -dl, -dx)
            total = total + moved.astype(f32)
        for i, pair in enumerate(chunk):
            sums[pair] = total[i * n_l : (i + 1) * n_l]

    pairs = [(dh, dy) for dh in range(n_h) for dy in range(n_y)]
    stacked = jnp.stack([sums[p] for p in pairs]).reshape(n_h, n_y, n_l, part_rows, d_block)
    stacked = jnp.take(stacked, (at_h - jnp.arange(n_h)) % n_h, axis=0)
    stacked = jnp.take(stacked, (at_y - jnp.arange(n_y)) % n_y, axis=1)
    ffn_sum = jnp.transpose(stacked, (3, 0, 2, 1, 4)).reshape(part_rows, n_sp * d_block)
    return layer_scaled(resid_alpha * own_normed.astype(f32) + 0.5 * ffn_sum, out_gain).astype(bf16)


def solution(mesh):
    in_specs = (
        P("sp", None),
        P("sp", None),
        P("sp", None),
        P("sp", None),
        P("sp"),
        P(),
        P(),
        P(None, "tp"),
        P(None, "tp"),
        P(None, "tp"),
        P(),
        P(),
        P("sp", "tp"),
        P("sp", "tp"),
        P("tp", "sp"),
        P(),
    )
    out_specs = P(("sp", "tp"), None)
    return jax.shard_map(body, mesh=mesh, in_specs=in_specs, out_specs=out_specs, check_vma=False)
```
